128 devices in a mesh: fs: 16 (over z, y), rep: 4 (over x), tp: 2 (over core).
Axes of the slice: x: 4, y: 4, z: 4, core: 2. Of those that a mesh axis runs over, the one named last changes fastest.
Arguments:
- query_input: bfloat16 [65536, 4096], P(('fs', 'rep')), may hold values from -6 to 6
- query_cotangent: bfloat16 [65536, 1024], P(('fs', 'rep'), 'tp'), may hold values from -0.0234375 to 0.0234375
- branch_output: bfloat16 [65536, 2048], P(('fs', 'rep')), may hold values from -6 to 6
- layer_cotangent: bfloat16 [65536, 4096], P(('fs', 'rep'), 'tp'), may hold values from -0.0234375 to 0.0234375
- query_weight: float32 [4096, 1024], P(('rep', 'fs'), 'tp'), may hold values from -0.09375 to 0.09375
- output_weight: float32 [2048, 4096], P(('rep', 'fs'), 'tp'), may hold values from -0.125 to 0.125
- query_basis: bfloat16 [4096, 512], P(('rep', 'fs')), may hold values from -0.09375 to 0.09375
- output_basis: bfloat16 [2048, 512], P(('rep', 'fs')), may hold values from -0.125 to 0.125
- query_first: float32 [512, 1024], P(('rep', 'fs'), 'tp'), may hold values from -20 to 20
- query_second: float32 [512, 1024], P(('rep', 'fs'), 'tp'), may hold values from 0.25 to 2
- output_first: float32 [512, 4096], P(('rep', 'fs'), 'tp'), may hold values from -20 to 20
- output_second: float32 [512, 4096], P(('rep', 'fs'), 'tp'), may hold values from 0.25 to 2
Outputs:
- query_update: float32 [4096, 1024], P(('rep', 'fs'), 'tp')
- output_update: float32 [2048, 4096], P(('rep', 'fs'), 'tp')
- query_first_next: float32 [512, 1024], P(('rep', 'fs'), 'tp')
- query_second_next: float32 [512, 1024], P(('rep', 'fs'), 'tp')
- output_first_next: float32 [512, 4096], P(('rep', 'fs'), 'tp')
- output_second_next: float32 [512, 4096], P(('rep', 'fs'), 'tp')
- query_copy: bfloat16 [4096, 1024], P('rep', 'tp')
- output_copy: bfloat16 [2048, 4096], P('rep', 'tp')
The draws below stay inside these ranges and needn't reach their ends.
All inputs are finite; a program needn't handle non-finite values.
Results may differ from the reference program's by a relative error of at most 0.0055.
Values may be sent and summed in bfloat16 or wider, within the bound.
A program may use at most 128 MiB of HBM per device.

```python
import math
import jax
import jax.numpy as jnp
from jax import lax

D = 4096
QKW = 1024
VW = 2048
R = 512
TOKENS = 65536


def first_moment(key, rows, cols):
    row_scale = 0.3 * 10.0 ** (jnp.arange(rows, dtype=jnp.float32) / (rows - 1))
    col_scale = jnp.exp(jax.random.uniform(jax.random.fold_in(key, 7), (cols,), jnp.float32, -0.7, 0.7))
    base = jnp.clip(jax.random.normal(jax.random.fold_in(key, 11), (rows, cols), jnp.float32), -3.0, 3.0)
    return base * row_scale[:, None] * col_scale[None, :]


def draw_query_first(key, part):
    return first_moment(key, R, QKW)


def draw_output_first(key, part):
    return first_moment(key, R, D)


def level_of(stream_key, extent, split, low, high):
    def one(dim, blocks):
        heights = jax.random.uniform(jax.random.fold_in(jax.random.fold_in(stream_key, 6), dim), (blocks,), jnp.float32, low / len(split), high / len(split))
        return jnp.repeat(jnp.exp(heights), extent[dim] // blocks).reshape((-1,) + (1,) * (len(extent) - dim - 1))

    loudness = one(*split[0])
    for cut in split[1:]:
        loudness = loudness * one(*cut)
    return loudness


def scatter_about(stream_key, dims, spread, reach, shards=(), kind=jnp.bfloat16):
    result = spread * jax.random.normal(stream_key, dims, jnp.float32)
    if shards:
        result = result * level_of(stream_key, dims, shards, -0.22, 0.18)
    return jnp.clip(result, -reach, reach).astype(kind)


def setup_inputs(seed: int = 0) -> dict:
    keys = jax.random.split(jax.random.key(seed), 13)
    query_input = scatter_about(keys[0], (TOKENS, D), 1.0, 6.0, ((0, 64),))
    query_cotangent = scatter_about(keys[1], (TOKENS, QKW), (TOKENS ** -0.5), 0.0234375, ((0, 64), (1, 2)))
    branch_output = scatter_about(keys[2], (TOKENS, VW), 1.0, 6.0, ((0, 64),))
    layer_cotangent = scatter_about(keys[3], (TOKENS, D), (TOKENS ** -0.5), 0.0234375, ((0, 64), (1, 2)))
    query_weight = scatter_about(keys[4], (D, QKW), D ** -0.5, 0.09375, ((0, 64), (1, 2)), jnp.float32)
    output_weight = scatter_about(keys[5], (VW, D), VW ** -0.5, 0.125, ((0, 64), (1, 2)), jnp.float32)
    query_basis = scatter_about(keys[6], (D, R), D ** -0.5, 0.09375, ((0, 64),))
    output_basis = scatter_about(keys[7], (VW, R), VW ** -0.5, 0.125, ((0, 64),))
    query_first = draw_query_first(jax.random.fold_in(keys[12], 71), 0)
    query_second = jnp.clip(jnp.exp(math.log(2.0) - 2.0794415 * jax.random.uniform(keys[9], (R, QKW), jnp.float32) ** level_of(keys[9], (R, QKW), ((0, 64), (1, 2)), -0.2, 0.2)), 0.25, 2.0)
    output_first = draw_output_first(jax.random.fold_in(keys[12], 71), 0)
    output_second = jnp.clip(jnp.exp(math.log(2.0) - 2.0794415 * jax.random.uniform(keys[11], (R, D), jnp.float32) ** level_of(keys[11], (R, D), ((0, 64), (1, 2)), -0.2, 0.2)), 0.25, 2.0)
    return dict(query_input=query_input, query_cotangent=query_cotangent, branch_output=branch_output, layer_cotangent=layer_cotangent, query_weight=query_weight, output_weight=output_weight, query_basis=query_basis, output_basis=output_basis, query_first=query_first, query_second=query_second, output_first=output_first, output_second=output_second)


beta_first = 0.6
beta_second = 0.8
step_rate = 0.01
small_eps = 1e-06

def project(inputs, basis, cotangent):
    inner = jnp.dot(inputs.astype(jnp.float32), basis.astype(jnp.float32), precision=lax.Precision.HIGHEST, preferred_element_type=jnp.float32)
    return jnp.dot(inner.T, cotangent.astype(jnp.float32), precision=lax.Precision.HIGHEST, preferred_element_type=jnp.float32)

def advance(first, second, projected, basis, weight):
    first_next = beta_first * first + (1.0 - beta_first) * projected
    second_next = beta_second * second + (1.0 - beta_second) * projected * projected
    normed = first_next / jnp.sqrt(second_next)
    scale = lax.rsqrt(jnp.mean(normed * normed) + small_eps)
    rounded = normed.astype(jnp.bfloat16)
    update = scale * jnp.dot(basis.astype(jnp.float32), rounded.astype(jnp.float32), precision=lax.Precision.HIGHEST, preferred_element_type=jnp.float32)
    copy = (weight - step_rate * update).astype(jnp.bfloat16)
    return (update, first_next, second_next, copy)

def reference(query_input, query_cotangent, branch_output, layer_cotangent, query_weight, output_weight, query_basis, output_basis, query_first, query_second, output_first, output_second):
    projected_q = project(query_input, query_basis, query_cotangent)
    projected_o = project(branch_output, output_basis, layer_cotangent)
    update_q, first_q, second_q, copy_q = advance(query_first, query_second, projected_q, query_basis, query_weight)
    update_o, first_o, second_o, copy_o = advance(output_first, output_second, projected_o, output_basis, output_weight)
    return (update_q, update_o, first_q, second_q, first_o, second_o, copy_q, copy_o)
```

```python
import functools

import jax
import jax.numpy as jnp
from jax import lax
from jax.experimental import pallas as pl
from jax.experimental.pallas import tpu as pltpu
from jax.sharding import Mesh
from jax.sharding import PartitionSpec as P

D = 4096
QKW = 1024
VW = 2048
R = 512
FS = ("fs_0", "fs_1")
REP_FS = ("rep", "fs_0", "fs_1")
FS_REP = ("fs_0", "fs_1", "rep")
AXES = ("rep", "fs_0", "fs_1")
ORDERS = (("fs_1", "fs_0", "rep"), ("fs_0", "rep", "fs_1"), ("rep", "fs_1", "fs_0"))

beta_first = 0.6
beta_second = 0.8
step_rate = 0.01
small_eps = 1e-06

MESH = pl.DeviceIdType.MESH
ANY = pl.BlockSpec(memory_space=pl.ANY)
VMEM = pl.BlockSpec(memory_space=pltpu.VMEM)
BF = jnp.bfloat16
F32 = jnp.float32
WIDE = 2688


def moments(first, second, projected):
    first_next = beta_first * first + (1.0 - beta_first) * projected
    second_next = beta_second * second + (1.0 - beta_second) * projected * projected
    return (first_next, second_next, first_next * lax.rsqrt(second_next))


def block_at(order, k, slot, coord):
    out = []
    for axis in AXES:
        if axis in order[:k]:
            out.append(slice(None))
        elif axis == order[k]:
            out.append(slot)
        else:
            out.append(coord[axis])
    return tuple(out)


def step_of(coord, axis, d):
    return lax.rem(coord[axis] + d, 4)


def sending(src, dst, ss, rs, at, axis, to):
    return pltpu.make_async_remote_copy(
        src_ref=src,
        dst_ref=dst,
        send_sem=ss.at[at],
        recv_sem=rs.at[at],
        device_id={axis: to},
        device_id_type=MESH,
    )


class Gather:
    def __init__(self, buf, order, k, low, high, coord, ss, rs, base):
        axis = order[k]
        right, left = step_of(coord, axis, 1), step_of(coord, axis, 3)

        def at(slot, half):
            return buf.at[block_at(order, k, slot, coord) + half]

        me = coord[axis]
        mk = lambda ref, n, to: sending(ref, ref, ss, rs, base + n, axis, to)
        self.first = [
            mk(at(me, low), 0, right),
            mk(at(me, high), 1, left),
            mk(at(me, high), 2, right),
            mk(at(me, low), 3, left),
        ]
        self.forward = [mk(at(left, low), 4, right), mk(at(right, high), 5, left)]

    def start(self):
        for c in self.first:
            c.start()

    def pass_on(self):
        for n in range(2):
            self.first[n].wait_recv()
            self.forward[n].start()

    def arrive(self):
        self.first[2].wait_recv()
        self.first[3].wait_recv()
        self.forward[0].wait_recv()
        self.forward[1].wait_recv()

    def sent(self):
        for c in self.first + self.forward:
            c.wait_send()


class Reduce:
    def __init__(self, buf, order, k, low, high, coord, ss, rs, base, from_left, from_right, mid_low, mid_high):
        axis = order[k]
        me = coord[axis]
        right, left, far = (step_of(coord, axis, d) for d in (1, 3, 2))
        self.at = lambda slot, half: block_at(order, k, slot, coord) + half
        self.buf, self.low, self.high = buf, low, high
        self.me, self.right, self.left = me, right, left
        self.from_left, self.from_right = from_left, from_right
        self.mid_low, self.mid_high = mid_low, mid_high
        n = len(block_at(order, k, me, coord))
        lead = sum(isinstance(i, slice) for i in block_at(order, k, me, coord))
        whole = (slice(None),) * lead
        start = low[-1].start

        def part(ref, half):
            h = half[-1]
            return ref.at[whole + (slice(None), slice(h.start - start, h.stop - start))]

        src = lambda slot, half: buf.at[self.at(slot, half)]
        mk = lambda s, d, i, to: sending(s, d, ss, rs, base + i, axis, to)
        self.first = [
            mk(src(far, low), mid_low, 0, right),
            mk(src(far, high), mid_high, 1, left),
            mk(src(right, high), part(from_left, high), 2, right),
            mk(src(left, low), part(from_right, low), 3, left),
        ]
        self.second = [
            mk(src(right, low), part(from_left, low), 4, right),
            mk(src(left, high), part(from_right, high), 5, left),
        ]

    def start(self):
        for c in self.first:
            c.start()

    def pass_on(self):
        self.first[0].wait_recv()
        i = self.at(self.right, self.low)
        self.buf[i] = (self.buf[i].astype(F32) + self.mid_low[...].astype(F32)).astype(BF)
        self.second[0].start()
        self.first[1].wait_recv()
        i = self.at(self.left, self.high)
        self.buf[i] = (self.buf[i].astype(F32) + self.mid_high[...].astype(F32)).astype(BF)
        self.second[1].start()

    def total(self):
        self.first[2].wait_recv()
        self.first[3].wait_recv()
        self.second[0].wait_recv()
        self.second[1].wait_recv()
        i = self.at(self.me, (slice(None), slice(self.low[-1].start, self.high[-1].stop)))
        own = self.buf[i].astype(F32)
        return i, own + self.from_left[...].astype(F32) + self.from_right[...].astype(F32)

    def sent(self):
        for c in self.first + self.second:
            c.wait_send()


def kernel(*refs):
    (x_hbm, cq_hbm, br_hbm, co_hbm, bq_hbm, bo_hbm, fq, sq, fo, so) = refs[:10]
    (fqn, sqn, fon, son, normed_out, sums_out) = refs[10:16]
    (x, br, cq, co, bq, bo, tq, to, p, n, proj, sums, psums) = refs[16:29]
    scratch = refs[29:29 + 36]
    (lsem, ags, agr, rss, rsr, ngs, ngr, psem_s, psem_r) = refs[65:]

    coord = {a: lax.axis_index(a) for a in AXES}
    core = lax.axis_index("tp")
    partner = 1 - core
    own = (coord["rep"], coord["fs_0"], coord["fs_1"])

    half = pl.ds(pl.multiple_of(core * 256, 256), 256)
    own_q = pltpu.make_async_copy(bq_hbm.at[:, half], bq.at[own], lsem.at[0])
    own_o = pltpu.make_async_copy(bo_hbm.at[:, half], bo.at[own], lsem.at[1])
    loads = [
        pltpu.make_async_copy(x_hbm, x, lsem.at[2]),
        pltpu.make_async_copy(br_hbm, br, lsem.at[3]),
        pltpu.make_async_copy(cq_hbm, cq, lsem.at[4]),
        pltpu.make_async_copy(co_hbm, co, lsem.at[5]),
    ]
    own_q.start()
    own_o.start()

    barrier = pltpu.get_barrier_semaphore()
    for axis in AXES:
        for d in (1, 3):
            pl.semaphore_signal(barrier, inc=1, device_id={axis: step_of(coord, axis, d)}, device_id_type=MESH)
    pl.semaphore_signal(barrier, inc=1, device_id={"tp": partner}, device_id_type=MESH)
    own_q.wait()
    own_o.wait()
    for c in loads:
        c.start()
    pl.semaphore_wait(barrier, 7)

    everything = slice(None)
    parts = ((bq, 0), (bq, 32), (bo, 0))
    done = []
    for k in range(3):
        phase = []
        for i, (buf, row) in enumerate(parts):
            low = (slice(row, row + 16), everything)
            high = (slice(row + 16, row + 32), everything)
            phase.append(Gather(buf, ORDERS[i], k, low, high, coord, ags, agr, (k * 3 + i) * 6))
        for g in phase:
            g.start()
        for g in phase:
            g.pass_on()
        for g in phase:
            g.arrive()
        done += phase

    for c in loads:
        c.wait()

    tiles = 256

    @pl.loop(0, 1024 // tiles)
    def _(t):
        rows = pl.ds(pl.multiple_of(t * tiles, tiles), tiles)
        acc = jnp.dot(x[rows, :], bq[...].reshape(4096, 256), preferred_element_type=F32)
        tq[core, :, rows] = acc.T.astype(BF)

    def to_partner(ref, i):
        return pltpu.make_async_remote_copy(
            src_ref=ref.at[core], dst_ref=ref.at[core], send_sem=psem_s.at[i], recv_sem=psem_r.at[i],
            device_id={"tp": partner}, device_id_type=MESH)

    swap_q = to_partner(tq, 0)
    swap_q.start()

    @pl.loop(0, 1024 // tiles)
    def _(t):
        rows = pl.ds(pl.multiple_of(t * tiles, tiles), tiles)
        acc = jnp.dot(br[rows, :], bo[...].reshape(2048, 256), preferred_element_type=F32)
        to[core, :, rows] = acc.T.astype(BF)

    swap_o = to_partner(to, 1)
    swap_o.start()

    def project(h):
        blocks = pl.ds(2 * h, 2)
        acc = jnp.dot(tq[h], cq[...], preferred_element_type=F32)
        p[blocks, :, :, :, 0:512] = acc.reshape(2, 4, 4, 8, 512).astype(BF)

        @pl.loop(0, 4)
        def _(t):
            cols = pl.ds(pl.multiple_of(t * 512, 512), 512)
            dest = pl.ds(pl.multiple_of(512 + t * 512, 512), 512)
            acc = jnp.dot(to[h], co[:, cols], preferred_element_type=F32)
            p[blocks, :, :, :, dest] = acc.reshape(2, 4, 4, 8, 512).astype(BF)

    project(core)
    swap_q.wait_recv()
    swap_o.wait_recv()
    project(partner)

    halves = (
        ((everything, slice(0, 512)), (everything, slice(512, 896))),
        ((everything, slice(896, 1408)), (everything, slice(1408, 1792))),
        ((everything, slice(1792, 2176)), (everything, slice(2176, 2560))),
    )
    for j, k in enumerate((2, 1, 0)):
        phase = []
        for i, (low, high) in enumerate(halves):
            bufs = scratch[(j * 3 + i) * 4:(j * 3 + i) * 4 + 4]
            phase.append(Reduce(p, ORDERS[i], k, low, high, coord, rss, rsr, (j * 3 + i) * 6, *bufs))
        for g in phase:
            g.start()
        for g in phase:
            g.pass_on()
        for i, g in enumerate(phase):
            at, total = g.total()
            if k:
                p[at] = total.astype(BF)
            else:
                proj[:, at[-1]] = total
        done += phase

    first_q, second_q, normed_q = moments(fq[...], sq[...], proj[:, 0:512])
    first_o, second_o, normed_o = moments(fo[...], so[...], proj[:, 512:2560])
    n[own + (everything, slice(0, 512))] = normed_q.astype(BF)
    n[own + (everything, slice(512, 2560))] = normed_o.astype(BF)
    lane = lax.broadcasted_iota(jnp.int32, (8, 128), 1)
    tile = jnp.zeros((8, 128), F32)
    for base, normed in ((0, normed_q), (3, normed_o)):
        rest = jnp.broadcast_to(jnp.sum(normed * normed, keepdims=True), (8, 128))
        for e in range(3):
            top = rest.astype(BF).astype(F32)
            tile = jnp.where(lane == base + e, top, tile)
            rest = rest - top
    n[own + (everything, slice(2560, 2688))] = tile.astype(BF)
    fqn[...] = first_q
    sqn[...] = second_q
    fon[...] = first_o
    son[...] = second_o

    halves = (
        ((everything, slice(0, 512)), (everything, slice(512, 896))),
        ((everything, slice(896, 1408)), (everything, slice(1408, 1792))),
        ((everything, slice(1792, 2304)), (everything, slice(2304, 2688))),
    )
    for k in range(3):
        phase = []
        for i, (low, high) in enumerate(halves):
            phase.append(Gather(n, ORDERS[i], k, low, high, coord, ngs, ngr, (k * 3 + i) * 6))
        for g in phase:
            g.start()
        for g in phase:
            g.pass_on()
        for g in phase:
            g.arrive()
        done += phase

    out = pltpu.make_async_copy(n, normed_out, lsem.at[6])
    out.start()
    sums[...] = jnp.sum(n[:, :, :, :, 2560:2688].astype(F32), axis=(0, 1, 2))
    swap_s = pltpu.make_async_remote_copy(
        src_ref=sums, dst_ref=psums, send_sem=psem_s.at[2], recv_sem=psem_r.at[2],
        device_id={"tp": partner}, device_id_type=MESH)
    swap_s.start()
    swap_s.wait_recv()
    both = sums[...] + psums[...]
    total_q = jnp.sum(jnp.where(lane < 3, both, 0.0), axis=1, keepdims=True)
    total_o = jnp.sum(jnp.where((lane >= 3) & (lane < 6), both, 0.0), axis=1, keepdims=True)
    scale_q = lax.rsqrt(total_q / (R * QKW) + small_eps)
    scale_o = lax.rsqrt(total_o / (R * D) + small_eps)
    sums_out[...] = jnp.where(lane == 0, scale_q, scale_o)
    for c in done:
        c.sent()
    for c in (swap_q, swap_o, swap_s):
        c.wait_send()
    out.wait()


def scratch_for_reduce():
    shapes = []
    widths = ((512, 384), (512, 384), (384, 384))
    for j, lead in enumerate(((4, 4), (4,), ())):
        for low, high in widths:
            shapes += [
                pltpu.VMEM(lead + (8, low + high), BF),
                pltpu.VMEM(lead + (8, low + high), BF),
                pltpu.VMEM(lead + (8, low), BF),
                pltpu.VMEM(lead + (8, high), BF),
            ]
    return shapes


def gathered_moments(x, cq, br, co, bq, bo, fq, sq, fo, so):
    sds = jax.ShapeDtypeStruct
    dma = pltpu.SemaphoreType.DMA
    return pl.pallas_call(
        kernel,
        out_shape=(
            sds((8, 512), F32), sds((8, 512), F32), sds((8, 2048), F32), sds((8, 2048), F32),
            sds((4, 4, 4, 8, WIDE), BF), sds((8, 128), F32),
        ),
        in_specs=[ANY] * 6 + [VMEM] * 4,
        out_specs=(VMEM, VMEM, VMEM, VMEM, ANY, VMEM),
        scratch_shapes=[
            pltpu.VMEM((1024, 4096), BF), pltpu.VMEM((1024, 2048), BF),
            pltpu.VMEM((1024, 512), BF), pltpu.VMEM((1024, 2048), BF),
            pltpu.VMEM((4, 4, 4, 64, 256), BF), pltpu.VMEM((4, 4, 4, 32, 256), BF),
            pltpu.VMEM((2, 256, 1024), BF), pltpu.VMEM((2, 256, 1024), BF),
            pltpu.VMEM((4, 4, 4, 8, WIDE), BF), pltpu.VMEM((4, 4, 4, 8, WIDE), BF),
            pltpu.VMEM((8, 2560), F32), pltpu.VMEM((8, 128), F32), pltpu.VMEM((8, 128), F32),
            *scratch_for_reduce(),
            dma((7,)), dma((54,)), dma((54,)), dma((54,)), dma((54,)), dma((54,)), dma((54,)),
            dma((3,)), dma((3,)),
        ],
        compiler_params=pltpu.CompilerParams(
            collective_id=0, has_side_effects=True, vmem_limit_bytes=60 * 1024 * 1024),
        name="moments_everywhere",
    )(x, cq, br, co, bq, bo, fq, sq, fo, so)


def gather_together(arrays, axis):
    ravelled = jnp.concatenate([a.reshape(-1) for a in arrays])
    lines, at, gathered = (lax.all_gather(ravelled, axis), 0, [])
    for a in arrays:
        tiles = lines[:, at : at + a.size].reshape(-1, a.shape[1])
        gathered.append(tiles)
        at += a.size
    return tuple(gathered)


def body(query_input, query_cotangent, branch_output, layer_cotangent, query_weight, output_weight,
         query_basis, output_basis, query_first, query_second, output_first, output_second):
    first_q, second_q, first_o, second_o, normed, scales = gathered_moments(
        query_input, query_cotangent, branch_output, layer_cotangent, query_basis, output_basis,
        query_first, query_second, output_first, output_second)
    rows = normed.reshape(R, WIDE)
    update_q = scales[0, 0] * jnp.dot(query_basis, rows[:, 0:512], preferred_element_type=F32)
    update_o = scales[0, 1] * jnp.dot(output_basis, rows[:, 512:2560], preferred_element_type=F32)
    query_copy, output_copy = gather_together(
        ((query_weight - step_rate * update_q).astype(BF), (output_weight - step_rate * update_o).astype(BF)), FS)
    return (update_q, update_o, first_q, second_q, first_o, second_o, query_copy, output_copy)


def solution(mesh):
    split = Mesh(
        mesh.devices.reshape(4, 4, mesh.shape["rep"], mesh.shape["tp"]),
        ("fs_0", "fs_1", "rep", "tp"),
    )
    tokens, rows = P(FS_REP, None), P(REP_FS, "tp")
    return jax.shard_map(
        body,
        mesh=split,
        in_specs=(tokens, P(FS_REP, "tp"), tokens, P(FS_REP, "tp"), rows, rows,
                  P(REP_FS, None), P(REP_FS, None), rows, rows, rows, rows),
        out_specs=(rows, rows, rows, rows, rows, rows, P("rep", "tp"), P("rep", "tp")),
        check_vma=False,
    )
```

```python
import functools

import jax
import jax.numpy as jnp
from jax import lax
from jax.experimental import pallas as pl
from jax.experimental.pallas import tpu as pltpu
from jax.sharding import Mesh
from jax.sharding import PartitionSpec as P

D = 4096
QKW = 1024
VW = 2048
R = 512
FS = ("fs_0", "fs_1")
REP_FS = ("rep", "fs_0", "fs_1")
FS_REP = ("fs_0", "fs_1", "rep")
AXES = ("rep", "fs_0", "fs_1")
ORDERS = (("fs_1", "fs_0", "rep"), ("fs_0", "rep", "fs_1"), ("rep", "fs_1", "fs_0"))

beta_first = 0.6
beta_second = 0.8
step_rate = 0.01
small_eps = 1e-06

MESH = pl.DeviceIdType.MESH
ANY = pl.BlockSpec(memory_space=pl.ANY)
VMEM = pl.BlockSpec(memory_space=pltpu.VMEM)
BF = jnp.bfloat16
F32 = jnp.float32
WIDE = 2688


def moments(first, second, projected):
    first_next = beta_first * first + (1.0 - beta_first) * projected
    second_next = beta_second * second + (1.0 - beta_second) * projected * projected
    return (first_next, second_next, first_next * lax.rsqrt(second_next))


def block_at(order, k, slot, coord):
    out = []
    for axis in [a for a in AXES if a in order]:
        if axis in order[:k]:
            out.append(slice(None))
        elif axis == order[k]:
            out.append(slot)
        else:
            out.append(coord[axis])
    return tuple(out)


def step_of(coord, axis, d):
    return lax.rem(coord[axis] + d, 4)


def sending(src, dst, ss, rs, at, axis, to):
    return pltpu.make_async_remote_copy(
        src_ref=src,
        dst_ref=dst,
        send_sem=ss.at[at],
        recv_sem=rs.at[at],
        device_id={axis: to},
        device_id_type=MESH,
    )


class Gather:
    def __init__(self, buf, order, k, low, high, coord, ss, rs, base):
        axis = order[k]
        right, left = step_of(coord, axis, 1), step_of(coord, axis, 3)

        def at(slot, half):
            return buf.at[block_at(order, k, slot, coord) + half]

        me = coord[axis]
        mk = lambda ref, n, to: sending(ref, ref, ss, rs, base + n, axis, to)
        self.first = [
            mk(at(me, low), 0, right),
            mk(at(me, high), 1, left),
            mk(at(me, high), 2, right),
            mk(at(me, low), 3, left),
        ]
        self.forward = [mk(at(left, low), 4, right), mk(at(right, high), 5, left)]

    def start(self):
        for c in self.first:
            c.start()

    def pass_on(self):
        for n in range(2):
            self.first[n].wait_recv()
            self.forward[n].start()

    def arrive(self):
        self.first[2].wait_recv()
        self.first[3].wait_recv()
        self.forward[0].wait_recv()
        self.forward[1].wait_recv()

    def sent(self):
        for c in self.first + self.forward:
            c.wait_send()


class Reduce:
    def __init__(self, buf, order, k, low, high, coord, ss, rs, base, from_left, from_right, mid_low, mid_high):
        axis = order[k]
        me = coord[axis]
        right, left, far = (step_of(coord, axis, d) for d in (1, 3, 2))
        self.at = lambda slot, half: block_at(order, k, slot, coord) + half
        self.buf, self.low, self.high = buf, low, high
        self.me, self.right, self.left = me, right, left
        self.from_left, self.from_right = from_left, from_right
        self.mid_low, self.mid_high = mid_low, mid_high
        n = len(block_at(order, k, me, coord))
        lead = sum(isinstance(i, slice) for i in block_at(order, k, me, coord))
        whole = (slice(None),) * lead
        start = low[-1].start

        def part(ref, half):
            h = half[-1]
            return ref.at[whole + (slice(None), slice(h.start - start, h.stop - start))]

        src = lambda slot, half: buf.at[self.at(slot, half)]
        mk = lambda s, d, i, to: sending(s, d, ss, rs, base + i, axis, to)
        self.first = [
            mk(src(far, low), mid_low, 0, right),
            mk(src(far, high), mid_high, 1, left),
            mk(src(right, high), part(from_left, high), 2, right),
            mk(src(left, low), part(from_right, low), 3, left),
        ]
        self.second = [
            mk(src(right, low), part(from_left, low), 4, right),
            mk(src(left, high), part(from_right, high), 5, left),
        ]

    def start(self):
        for c in self.first:
            c.start()

    def pass_on(self):
        self.first[0].wait_recv()
        i = self.at(self.right, self.low)
        self.buf[i] = (self.buf[i].astype(F32) + self.mid_low[...].astype(F32)).astype(BF)
        self.second[0].start()
        self.first[1].wait_recv()
        i = self.at(self.left, self.high)
        self.buf[i] = (self.buf[i].astype(F32) + self.mid_high[...].astype(F32)).astype(BF)
        self.second[1].start()

    def total(self):
        self.first[2].wait_recv()
        self.first[3].wait_recv()
        self.second[0].wait_recv()
        self.second[1].wait_recv()
        i = self.at(self.me, (slice(None), slice(self.low[-1].start, self.high[-1].stop)))
        own = self.buf[i].astype(F32)
        return i, own + self.from_left[...].astype(F32) + self.from_right[...].astype(F32)

    def sent(self):
        for c in self.first + self.second:
            c.wait_send()


def kernel(*refs):
    (x_hbm, cq_hbm, br_hbm, co_hbm, bq_hbm, bo_hbm, wq_in, wo_in, fq, sq, fo, so) = refs[:12]
    (proj, scales_out, normed_out, bq_out, bo_out, wq_out, wo_out) = refs[12:19]
    (x, br, cq, co, bq, bo, bq2, bo2, wq, wo, tq, to, p, n, sums, psums) = refs[19:35]
    scratch = refs[35:71]
    (lsem, ags, agr, rss, rsr, ngs, ngr, wgs, wgr, psem_s, psem_r) = refs[71:]

    coord = {a: lax.axis_index(a) for a in AXES}
    core = lax.axis_index("tp")
    partner = 1 - core
    own = (coord["rep"], coord["fs_0"], coord["fs_1"])
    everything = slice(None)

    half = pl.ds(pl.multiple_of(core * 256, 256), 256)
    other = pl.ds(pl.multiple_of(partner * 256, 256), 256)
    own_q = pltpu.make_async_copy(bq_hbm.at[:, half], bq.at[own], lsem.at[0])
    own_o = pltpu.make_async_copy(bo_hbm.at[:, half], bo.at[own], lsem.at[1])
    loads = [
        pltpu.make_async_copy(x_hbm, x, lsem.at[2]),
        pltpu.make_async_copy(br_hbm, br, lsem.at[3]),
        pltpu.make_async_copy(cq_hbm, cq, lsem.at[4]),
        pltpu.make_async_copy(co_hbm, co, lsem.at[5]),
    ]
    own_q.start()
    own_o.start()

    barrier = pltpu.get_barrier_semaphore()
    for axis in AXES:
        for d in (1, 3):
            pl.semaphore_signal(barrier, inc=1, device_id={axis: step_of(coord, axis, d)}, device_id_type=MESH)
    pl.semaphore_signal(barrier, inc=1, device_id={"tp": partner}, device_id_type=MESH)
    own_q.wait()
    own_o.wait()
    for c in loads:
        c.start()
    pl.semaphore_wait(barrier, 7)
    done = []

    def gathers(k, parts, ss, rs, orders=ORDERS):
        phase = []
        for i, (buf, low, high) in enumerate(parts):
            phase.append(Gather(buf, orders[i], k, low, high, coord, ss, rs, (k * len(parts) + i) * 6))
        for g in phase:
            g.start()
        done.extend(phase)
        return phase

    def pass_on(phase):
        for g in phase:
            g.pass_on()

    def arrive(phase):
        for g in phase:
            g.arrive()

    def rows_of(buf, row):
        return (buf, (slice(row, row + 16), everything), (slice(row + 16, row + 32), everything))

    def cols_of(buf, a, b, c):
        return (buf, (everything, slice(a, b)), (everything, slice(b, c)))

    for k in range(3):
        phase = gathers(k, (rows_of(bq, 0), rows_of(bq, 32), rows_of(bo, 0)), ags, agr)
        if k == 0:
            wq[own[1:]] = wq_in[...].astype(BF)
            wo[own[1:]] = wo_in[...].astype(BF)
        pass_on(phase)
        arrive(phase)

    weights = (cols_of(wo, 0, 768, 1536), cols_of(wo, 1536, 1792, 2048), cols_of(wq, 0, 256, 512))
    turns = (("fs_0", "fs_1"), ("fs_1", "fs_0"), ("fs_1", "fs_0"))
    carried = gathers(0, weights, wgs, wgr, turns)

    for c in loads:
        c.wait()

    tiles = 256

    @pl.loop(0, 1024 // tiles)
    def _(t):
        rows = pl.ds(pl.multiple_of(t * tiles, tiles), tiles)
        acc = jnp.dot(x[rows, :], bq[...].reshape(4096, 256), preferred_element_type=F32)
        tq[core, :, rows] = acc.T.astype(BF)

    def to_partner(src, dst, i):
        return pltpu.make_async_remote_copy(
            src_ref=src, dst_ref=dst, send_sem=psem_s.at[i], recv_sem=psem_r.at[i],
            device_id={"tp": partner}, device_id_type=MESH)

    swap_q = to_partner(tq.at[core], tq.at[core], 0)
    swap_q.start()
    pass_on(carried)

    @pl.loop(0, 1024 // tiles)
    def _(t):
        rows = pl.ds(pl.multiple_of(t * tiles, tiles), tiles)
        acc = jnp.dot(br[rows, :], bo[...].reshape(2048, 256), preferred_element_type=F32)
        to[core, :, rows] = acc.T.astype(BF)

    swap_o = to_partner(to.at[core], to.at[core], 1)
    swap_o.start()
    arrive(carried)
    carried = gathers(1, weights, wgs, wgr, turns)
    swap_bq = to_partner(bq.at[own[0]], bq2, 3)
    swap_bo = to_partner(bo.at[own[0]], bo2, 4)
    swap_bq.start()
    swap_bo.start()

    def project(h, t, c, a, b, at):
        acc = jnp.dot(t[h], c[:, a:b], preferred_element_type=F32)
        p[pl.ds(2 * h, 2), :, :, :, at:at + b - a] = acc.reshape(2, 4, 4, 8, b - a).astype(BF)

    halves = (
        ((everything, slice(0, 512)), (everything, slice(512, 896))),
        ((everything, slice(896, 1408)), (everything, slice(1408, 1792))),
        ((everything, slice(1792, 2176)), (everything, slice(2176, 2560))),
    )

    def reduces(j, i):
        low, high = halves[i]
        bufs = scratch[(j * 3 + i) * 4:(j * 3 + i) * 4 + 4]
        g = Reduce(p, ORDERS[i], 2 - j, low, high, coord, rss, rsr, (j * 3 + i) * 6, *bufs)
        g.start()
        done.append(g)
        return g

    project(core, tq, cq, 0, 512, 0)
    swap_q.wait_recv()
    project(partner, tq, cq, 0, 512, 0)
    project(core, to, co, 0, 384, 512)
    swap_o.wait_recv()
    project(partner, to, co, 0, 384, 512)
    phase = [reduces(0, 0)]
    for i, (a, b) in enumerate(((384, 1280), (1280, 2048))):
        for h in range(2):
            project(h, to, co, a, b, 512 + a)
        phase.append(reduces(0, i + 1))
    for g in phase:
        g.pass_on()
    for j in range(3):
        later = []
        for i, g in enumerate(phase):
            at, total = g.total()
            if j < 2:
                p[at] = total.astype(BF)
                later.append(reduces(j + 1, i))
            else:
                proj[:, at[-1]] = total
        if j == 0:
            pass_on(carried)
        phase = later
        for g in phase:
            g.pass_on()

    first_q, second_q, normed_q = moments(fq[...], sq[...], proj[:, 0:512])
    first_o, second_o, normed_o = moments(fo[...], so[...], proj[:, 512:2560])
    n[own + (everything, slice(0, 512))] = normed_q.astype(BF)
    n[own + (everything, slice(512, 2560))] = normed_o.astype(BF)
    lane = lax.broadcasted_iota(jnp.int32, (8, 128), 1)
    tile = jnp.zeros((8, 128), F32)
    for base, normed in ((0, normed_q), (3, normed_o)):
        rest = jnp.broadcast_to(jnp.sum(normed * normed, keepdims=True), (8, 128))
        for e in range(3):
            top = rest.astype(BF).astype(F32)
            tile = jnp.where(lane == base + e, top, tile)
            rest = rest - top
    n[own + (everything, slice(2560, 2688))] = tile.astype(BF)

    swap_bq.wait_recv()
    swap_bo.wait_recv()
    outs = [
        pltpu.make_async_copy(bq.at[own[0]], bq_out.at[:, :, :, half], lsem.at[7]),
        pltpu.make_async_copy(bo.at[own[0]], bo_out.at[:, :, :, half], lsem.at[8]),
        pltpu.make_async_copy(bq2, bq_out.at[:, :, :, other], lsem.at[9]),
        pltpu.make_async_copy(bo2, bo_out.at[:, :, :, other], lsem.at[10]),
    ]
    late = [pltpu.make_async_copy(wq, wq_out, lsem.at[11]), pltpu.make_async_copy(wo, wo_out, lsem.at[12])]

    for k in range(3):
        phase = gathers(k, (cols_of(n, 0, 512, 896), cols_of(n, 896, 1408, 1792), cols_of(n, 1792, 2304, 2688)), ngs, ngr)
        if k == 0:
            for c in outs:
                c.start()
        pass_on(phase)
        if k == 2:
            arrive(carried)
            for c in late:
                c.start()
        arrive(phase)

    out = pltpu.make_async_copy(n, normed_out, lsem.at[6])
    out.start()
    sums[...] = jnp.sum(n[:, :, :, :, 2560:2688].astype(F32), axis=(0, 1, 2))
    swap_s = to_partner(sums, psums, 2)
    swap_s.start()
    swap_s.wait_recv()
    both = sums[...] + psums[...]
    total_q = jnp.sum(jnp.where(lane < 3, both, 0.0), axis=1, keepdims=True)
    total_o = jnp.sum(jnp.where((lane >= 3) & (lane < 6), both, 0.0), axis=1, keepdims=True)
    scale_q = lax.rsqrt(total_q / (R * QKW) + small_eps)
    scale_o = lax.rsqrt(total_o / (R * D) + small_eps)
    scales_out[...] = jnp.where(lane == 0, scale_q, scale_o)
    for c in done:
        c.sent()
    for c in (swap_q, swap_o, swap_s, swap_bq, swap_bo):
        c.wait_send()
    for c in [out] + outs + late:
        c.wait()


def finish(n_hbm, bq_hbm, bo_hbm, wq_hbm, wo_hbm, proj, scales, fq, sq, fo, so,
           uq, uo, fqn, sqn, fon, son, cq_hbm, co_hbm,
           n, bq, bo, wq, wo, pq, po, cq, co, sem):
    fs = lax.axis_index("fs_0") * 4 + lax.axis_index("fs_1")
    load = lambda src, dst, i: pltpu.make_async_copy(src, dst, sem.at[i])
    loads = [
        load(n_hbm, n, 0),
        load(bq_hbm, bq, 1), load(wq_hbm, wq, 2), load(bo_hbm, bo, 3), load(wo_hbm, wo, 4),
    ]
    for c in loads:
        c.start()
    fqn[...], sqn[...], _ = moments(fq[...], sq[...], proj[:, 0:512])
    fon[...], son[...], _ = moments(fo[...], so[...], proj[:, 512:2560])
    scale_q = scales[0:1, 0:1]
    scale_o = scales[0:1, 1:2]
    outs = []
    loads[0].wait()
    loads[1].wait()
    loads[2].wait()
    for t in range(4):
        r = slice(t * 256, t * 256 + 256)
        acc = scale_q * jnp.dot(bq[r, :], n[:, 0:512], preferred_element_type=F32)
        pq[r, :] = acc
        cq[r, :] = (wq[r, :].astype(F32) - step_rate * acc).astype(BF)
        outs.append(load(cq.at[r], cq_hbm.at[r], 5 + t))
        outs[-1].start()
    uq[...] = pq[pl.ds(pl.multiple_of(fs * 64, 64), 64), :]
    loads[3].wait()
    loads[4].wait()
    for t in range(4):
        c = slice(t * 512, t * 512 + 512)
        acc = scale_o * jnp.dot(bo[...], n[:, 512 + t * 512:1024 + t * 512], preferred_element_type=F32)
        po[:, c] = acc
        co[:, c] = (wo[:, c].astype(F32) - step_rate * acc).astype(BF)
        outs.append(load(co.at[:, c], co_hbm.at[:, c], 9 + t))
        outs[-1].start()
    uo[...] = po[pl.ds(pl.multiple_of(fs * 32, 32), 32), :]
    for c in outs:
        c.wait()


def scratch_for_reduce():
    shapes = []
    widths = ((512, 384), (512, 384), (384, 384))
    for j, lead in enumerate(((4, 4), (4,), ())):
        for low, high in widths:
            shapes += [
                pltpu.VMEM(lead + (8, low + high), BF),
                pltpu.VMEM(lead + (8, low + high), BF),
                pltpu.VMEM(lead + (8, low), BF),
                pltpu.VMEM(lead + (8, high), BF),
            ]
    return shapes


def gathered_moments(*args):
    sds = jax.ShapeDtypeStruct
    dma = pltpu.SemaphoreType.DMA
    return pl.pallas_call(
        kernel,
        out_shape=(
            sds((8, 2560), F32), sds((8, 128), F32), sds((4, 4, 4, 8, WIDE), BF),
            sds((4, 4, 64, 512), BF), sds((4, 4, 32, 512), BF), sds((4, 4, 64, 512), BF), sds((4, 4, 32, 2048), BF),
        ),
        in_specs=[ANY] * 6 + [VMEM] * 6,
        out_specs=(VMEM, VMEM, ANY, ANY, ANY, ANY, ANY),
        scratch_shapes=[
            pltpu.VMEM((1024, 4096), BF), pltpu.VMEM((1024, 2048), BF),
            pltpu.VMEM((1024, 512), BF), pltpu.VMEM((1024, 2048), BF),
            pltpu.VMEM((4, 4, 4, 64, 256), BF), pltpu.VMEM((4, 4, 4, 32, 256), BF),
            pltpu.VMEM((4, 4, 64, 256), BF), pltpu.VMEM((4, 4, 32, 256), BF),
            pltpu.VMEM((4, 4, 64, 512), BF), pltpu.VMEM((4, 4, 32, 2048), BF),
            pltpu.VMEM((2, 256, 1024), BF), pltpu.VMEM((2, 256, 1024), BF),
            pltpu.VMEM((4, 4, 4, 8, WIDE), BF), pltpu.VMEM((4, 4, 4, 8, WIDE), BF),
            pltpu.VMEM((8, 128), F32), pltpu.VMEM((8, 128), F32),
            *scratch_for_reduce(),
            dma((13,)), dma((54,)), dma((54,)), dma((54,)), dma((54,)), dma((54,)), dma((54,)),
            dma((36,)), dma((36,)), dma((5,)), dma((5,)),
        ],
        compiler_params=pltpu.CompilerParams(
            collective_id=0, has_side_effects=True, vmem_limit_bytes=60 * 1024 * 1024),
        name="moments_everywhere",
    )(*args)


def updates(*args):
    sds = jax.ShapeDtypeStruct
    return pl.pallas_call(
        finish,
        out_shape=(
            sds((64, 512), F32), sds((32, 2048), F32),
            sds((8, 512), F32), sds((8, 512), F32), sds((8, 2048), F32), sds((8, 2048), F32),
            sds((1024, 512), BF), sds((512, 2048), BF),
        ),
        in_specs=[ANY] * 5 + [VMEM] * 6,
        out_specs=(VMEM,) * 6 + (ANY, ANY),
        scratch_shapes=[
            pltpu.VMEM((R, WIDE), BF), pltpu.VMEM((1024, 512), BF), pltpu.VMEM((512, 512), BF),
            pltpu.VMEM((1024, 512), BF), pltpu.VMEM((512, 2048), BF),
            pltpu.VMEM((1024, 512), F32), pltpu.VMEM((512, 2048), F32),
            pltpu.VMEM((1024, 512), BF), pltpu.VMEM((512, 2048), BF),
            pltpu.SemaphoreType.DMA((13,)),
        ],
        compiler_params=pltpu.CompilerParams(vmem_limit_bytes=60 * 1024 * 1024),
        name="updates",
    )(*args)


def body(query_input, query_cotangent, branch_output, layer_cotangent, query_weight, output_weight,
         query_basis, output_basis, query_first, query_second, output_first, output_second):
    state = (query_first, query_second, output_first, output_second)
    proj, scales, normed, bq, bo, wq, wo = gathered_moments(
        query_input, query_cotangent, branch_output, layer_cotangent, query_basis, output_basis,
        query_weight, output_weight, *state)
    return updates(
        normed.reshape(R, WIDE), bq.reshape(1024, 512), bo.reshape(512, 512), wq.reshape(1024, 512),
        wo.reshape(512, 2048), proj, scales, *state)


def solution(mesh):
    split = Mesh(
        mesh.devices.reshape(4, 4, mesh.shape["rep"], mesh.shape["tp"]),
        ("fs_0", "fs_1", "rep", "tp"),
    )
    tokens, rows = P(FS_REP, None), P(REP_FS, "tp")
    return jax.shard_map(
        body,
        mesh=split,
        in_specs=(tokens, P(FS_REP, "tp"), tokens, P(FS_REP, "tp"), rows, rows,
                  P(REP_FS, None), P(REP_FS, None), rows, rows, rows, rows),
        out_specs=(rows, rows, rows, rows, rows, rows, P("rep", "tp"), P("rep", "tp")),
        check_vma=False,
    )
```
